32 devices in a mesh: fs: 8 (over z, y), tp: 4 (over x, core).
Axes of the slice: x: 2, y: 2, z: 4, core: 2. Of those that a mesh axis runs over, the one named last changes fastest.
Arguments:
- tokens: bfloat16 [4096, 2048], P(('fs', 'tp')), may hold values from -6 to 6
- gate_proj: bfloat16 [2048, 512], P('fs', 'tp'), may hold values from -0.125 to 0.125
- signal_proj: bfloat16 [2048, 512], P('fs', 'tp'), may hold values from -1.5467961 to 1.5467961
- spatial: bfloat16 [4, 128, 128], replicated, may hold values from -0.5 to 0.5
- signal_gain: bfloat16 [512], P('tp'), may hold values from 0.099609375 to 1.8984375
- mixer_out: bfloat16 [512, 2048], P('tp', 'fs'), may hold values from -0.25 to 0.25
- mixer_gain: bfloat16 [2048], replicated, may hold values from 0.099609375 to 1.8984375
- ffn_gate: bfloat16 [2048, 5632], P('fs', 'tp'), may hold values from -0.125 to 0.125
- ffn_value: bfloat16 [2048, 5632], P('fs', 'tp'), may hold values from -0.125 to 0.125
- conv_taps: bfloat16 [3, 5632], P(None, 'tp'), may hold values from -3.5 to 3.5
- ffn_down: bfloat16 [5632, 2048], P('tp', 'fs'), may hold values from -0.078125 to 0.078125
- output_gain: bfloat16 [2048], replicated, may hold values from 0.099609375 to 1.8984375
Outputs:
- result: bfloat16 [4096, 2048], P(('fs', 'tp'))
The draws below stay inside these ranges and needn't reach their ends.
All inputs are finite; a program needn't handle non-finite values.
Results may differ from the reference program's by a relative error of at most 0.01.
Values may be sent and summed in bfloat16 or wider, within the bound.
A program may use at most 64 MiB of HBM per device.

```python
import math
import jax
import jax.numpy as jnp
from jax import lax

D = 2048
MIX_WIDTH = 512
HEAD_SIZE = 128
HEADS = 4
BLOCK = 128
SEGMENT = 64
FF = 5632
SEQ = 512
TOKENS = 4096
N_FS = 8
N_TP = 4


def draw_signal_proj(key, part):
    first_key, second_key = jax.random.split(jax.random.fold_in(key, 17))
    column = jnp.arange(MIX_WIDTH, dtype=jnp.float32) / MIX_WIDTH
    jitter = jnp.exp(jax.random.uniform(second_key, (MIX_WIDTH,), jnp.float32, -0.35, 0.35))
    entries = jnp.clip(jax.random.normal(first_key, (D, MIX_WIDTH), jnp.float32), -6.0, 6.0)
    rising = 4.0 ** column
    scales = rising * jitter / jnp.sqrt(jnp.float32(D))
    return (entries * scales[None, :]).astype(jnp.bfloat16)


def levels(stream_key, dims, cuts, low, top_value):
    def one(axis_at, blocks):
        draws = jax.random.uniform(jax.random.fold_in(jax.random.fold_in(stream_key, 6), axis_at), (blocks,), jnp.float32, low / len(cuts), top_value / len(cuts))
        return jnp.repeat(jnp.exp(draws), dims[axis_at] // blocks).reshape((-1,) + (1,) * (len(dims) - axis_at - 1))

    factor_of = one(*cuts[0])
    for cut in cuts[1:]:
        factor_of = factor_of * one(*cut)
    return factor_of


def scatter_about(key, dims, scale, most, cuts=(), kind=jnp.bfloat16):
    drawn = scale * jax.random.normal(key, dims, jnp.float32)
    if cuts:
        drawn = drawn * levels(key, dims, cuts, -0.22, 0.18)
    return jnp.clip(drawn, -most, most).astype(kind)


def setup_inputs(seed: int = 0) -> dict:
    seeds = jax.random.split(jax.random.key(seed), 13)
    return {
        "tokens": scatter_about(seeds[0], (TOKENS, D), 1.0, 6.0, ((0, 32),)),
        "gate_proj": scatter_about(seeds[1], (D, MIX_WIDTH), D ** -0.5, 0.125, ((0, 8), (1, 4))),
        "signal_proj": draw_signal_proj(jax.random.fold_in(seeds[12], 71), 0),
        "spatial": scatter_about(seeds[3], (HEADS, BLOCK, BLOCK), BLOCK ** -0.5, 0.5),
        "signal_gain": jnp.clip(1.0 + 0.18 * jax.random.normal(seeds[4], (MIX_WIDTH,), jnp.float32), 0.099609375, 1.8984375).astype(jnp.bfloat16),
        "mixer_out": scatter_about(seeds[5], (MIX_WIDTH, D), MIX_WIDTH ** -0.5, 0.25, ((0, 4), (1, 8))),
        "mixer_gain": jnp.clip(1.0 + 0.18 * jax.random.normal(seeds[6], (D,), jnp.float32), 0.099609375, 1.8984375).astype(jnp.bfloat16),
        "ffn_gate": scatter_about(seeds[7], (D, FF), D ** -0.5, 0.125, ((0, 8), (1, 4))),
        "ffn_value": scatter_about(seeds[8], (D, FF), D ** -0.5, 0.125, ((0, 8), (1, 4))),
        "conv_taps": scatter_about(seeds[9], (3, FF), 3 ** -0.5, 3.5, ((1, 4),)),
        "ffn_down": scatter_about(seeds[10], (FF, D), FF ** -0.5, 0.078125, ((0, 4), (1, 8))),
        "output_gain": jnp.clip(1.0 + 0.18 * jax.random.normal(seeds[11], (D,), jnp.float32), 0.099609375, 1.8984375).astype(jnp.bfloat16),
    }


EPSILON = 1e-05
RESIDUAL_SCALE = math.sqrt(2.0)

def normalize(values):
    row_mean = lax.optimization_barrier(jnp.mean(values, axis=-1, keepdims=True))
    centred = values - row_mean
    spread = lax.optimization_barrier(jnp.mean(centred * centred, axis=-1, keepdims=True))
    return centred * lax.rsqrt(spread + EPSILON)

def one_sequence(sequence, gate_proj, signal_proj, spatial, signal_gain, mixer_out, mixer_gain, ffn_gate, ffn_value, conv_taps, ffn_down, output_gain):
    residual = sequence.astype(jnp.float32)
    mix_input = normalize(residual).astype(jnp.bfloat16)
    branch_gate = jax.nn.gelu(jnp.dot(mix_input, gate_proj, preferred_element_type=jnp.float32))
    branch_signal = jax.nn.gelu(jnp.dot(mix_input, signal_proj, preferred_element_type=jnp.float32))
    spatial_input = (normalize(branch_signal) * signal_gain.astype(jnp.float32)).astype(jnp.bfloat16)
    segment_ids = jnp.arange(BLOCK) // SEGMENT
    allowed = segment_ids[None, :] <= segment_ids[:, None]
    masked = jnp.where(allowed[None], spatial, jnp.zeros_like(spatial))
    blocks = spatial_input.reshape(SEQ // BLOCK, BLOCK, HEADS, HEAD_SIZE)
    mixed = jnp.einsum('hij,njhd->nihd', masked.astype(jnp.float32), blocks.astype(jnp.float32)).reshape(SEQ, MIX_WIDTH)
    gated = (branch_gate * mixed).astype(jnp.bfloat16)
    mix_out = jnp.dot(gated, mixer_out, preferred_element_type=jnp.float32)
    middle = (normalize(RESIDUAL_SCALE * residual + mix_out) * mixer_gain.astype(jnp.float32)).astype(jnp.bfloat16)
    middle_wide = middle.astype(jnp.float32)
    ffn_input = normalize(middle_wide).astype(jnp.bfloat16)
    gate_pre = jnp.dot(ffn_input, ffn_gate, preferred_element_type=jnp.float32)
    value_pre = jnp.dot(ffn_input, ffn_value, preferred_element_type=jnp.float32)
    taps = conv_taps.astype(jnp.float32)
    shifted_one = jnp.concatenate([jnp.zeros((1, FF), jnp.float32), gate_pre[:-1]], axis=0)
    shifted_two = jnp.concatenate([jnp.zeros((2, FF), jnp.float32), gate_pre[:-2]], axis=0)
    conv_gate = taps[0] * shifted_two + taps[1] * shifted_one + taps[2] * gate_pre
    hidden = (jax.nn.silu(conv_gate) * value_pre).astype(jnp.bfloat16)
    group_width = FF // N_TP
    ffn_out = jnp.zeros((SEQ, D), jnp.float32)
    for group in range(N_TP):
        partial_sum = jnp.dot(hidden[:, group * group_width:(group + 1) * group_width], ffn_down[group * group_width:(group + 1) * group_width], preferred_element_type=jnp.float32)
        rounded = lax.optimization_barrier(partial_sum.astype(jnp.bfloat16))
        ffn_out = ffn_out + rounded.astype(jnp.float32)
    return (normalize(RESIDUAL_SCALE * middle_wide + ffn_out) * output_gain.astype(jnp.float32)).astype(jnp.bfloat16)

def reference(tokens, gate_proj, signal_proj, spatial, signal_gain, mixer_out, mixer_gain, ffn_gate, ffn_value, conv_taps, ffn_down, output_gain):
    sequences = tokens.reshape(N_FS, SEQ, D)

    def apply_layer(sequence):
        return one_sequence(sequence, gate_proj, signal_proj, spatial, signal_gain, mixer_out, mixer_gain, ffn_gate, ffn_value, conv_taps, ffn_down, output_gain)
    outputs = lax.map(apply_layer, sequences)
    return outputs.reshape(TOKENS, D)
```

```python
import functools
import math

import jax
import jax.numpy as jnp
from jax import lax
from jax.experimental import pallas as pl
from jax.experimental.pallas import tpu as pltpu
from jax.sharding import PartitionSpec as P

MIX_WIDTH = 512
HEAD_SIZE = 128
BLOCK = 128
SEGMENT = 64
LANES = 128
EPSILON = 1e-05
RESIDUAL_SCALE = math.sqrt(2.0)
MESH = pl.DeviceIdType.MESH
F32 = jnp.float32
BF16 = jnp.bfloat16


def normalize(values):
    row_mean = jnp.mean(values, axis=-1, keepdims=True)
    centred = values - row_mean
    spread = jnp.mean(centred * centred, axis=-1, keepdims=True)
    return centred * lax.rsqrt(spread + EPSILON)


def kernel(
    nz, ny, nx,
    tok, gs, mo, gv, dn, spatial, sgain, mgain, taps, ogain,
    out,
    gsb, mob, gvb, dnb, xin, stat, pm, prc, abm, pxr, mid, hin, hid, pb, rb, ab, xr, zb, zr,
    loc_sem, zs, zrs, ys, yrs, ts, trs,
):
    R, D = tok.shape
    C = mo.shape[0]
    cw = mo.shape[1]
    W = dn.shape[1]
    f = lax.axis_index("fs")
    t = lax.axis_index("tp")
    z, y = f // ny, f % ny
    x, c = t // 2, t % 2
    q = z % 2
    seq = nx * 2 * R

    def zpeer(d):
        return (lax.rem(z + d, nz) * ny + y, t)

    def ypeer(d):
        return (z * ny + lax.rem(y + d, ny), t)

    def xpeer(d):
        return (f, lax.rem(x + d, nx) * 2 + c)

    cpeer = (f, x * 2 + 1 - c)
    ppeer = ((z + 1 - 2 * q) * ny + y, t)

    def zsrc(d):
        return lax.rem(z + nz - d, nz)

    def ysrc(d):
        return lax.rem(y + ny - d, ny)

    def xsrc(d):
        return lax.rem(x + nx - d, nx)

    pending = []

    def send(src, dst, ssem, rsem, to):
        copy = pltpu.make_async_remote_copy(
            src_ref=src, dst_ref=dst, send_sem=ssem, recv_sem=rsem, device_id=to, device_id_type=MESH
        )
        copy.start()
        pending.append(copy)

    def arrived(dst, ssem, rsem, to):
        pltpu.make_async_remote_copy(
            src_ref=dst, dst_ref=dst, send_sem=ssem, recv_sem=rsem, device_id=to, device_id_type=MESH
        ).wait_recv()

    barrier = pltpu.get_barrier_semaphore()
    peers = [zpeer(d) for d in range(1, nz)] + [ypeer(d) for d in range(1, ny)]
    peers += [xpeer(d) for d in range(1, nx)] + [cpeer]
    for p in peers:
        pl.semaphore_signal(barrier, inc=1, device_id=p, device_id_type=MESH)
    pl.semaphore_wait(barrier, len(peers))

    bufs = (gsb, mob, gvb, dnb)

    def local(a, zz):
        return (gs, mo, gv.at[zz % 2], dn.at[zz % 2])[a]

    def issue(a):
        own = pltpu.make_async_copy(local(a, z), bufs[a].at[z, y], loc_sem.at[a])
        own.start()
        for d in range(1, nz):
            to = zpeer(d)
            send(local(a, lax.rem(z + d, nz)), bufs[a].at[z, y], zs.at[a, d], zrs.at[a, d], to)
        for e in range(1, ny):
            send(local(a, z), bufs[a].at[z, y], ys.at[a, 0, e], yrs.at[a, 0, e], ypeer(e))
        own.wait()

    def relay(a, d):
        zz = zsrc(d)
        arrived(bufs[a].at[zz, y], zs.at[a, d], zrs.at[a, d], zpeer(d))
        for e in range(1, ny):
            send(bufs[a].at[zz, y], bufs[a].at[zz, y], ys.at[a, d, e], yrs.at[a, d, e], ypeer(e))

    def complete(a, d):
        zz = zsrc(d)
        for e in range(1, ny):
            yy = ysrc(e)
            arrived(bufs[a].at[zz, yy], ys.at[a, d, e], yrs.at[a, d, e], ypeer(e))

    tslot = [0]

    def tsem():
        k = tslot[0]
        tslot[0] += 1
        return ts.at[k], trs.at[k]

    issue(0)
    issue(1)
    issue(2)

    xin[x, c] = normalize(tok[...].astype(F32)).astype(BF16)
    s1 = [tsem() for _ in range(nx)]
    s2 = [tsem() for _ in range(nx)]
    for d in range(1, nx):
        send(xin.at[x, c], xin.at[x, c], *s1[d], xpeer(d))
    send(xin.at[x, c], xin.at[x, c], *s2[0], cpeer)
    for a in (0, 1):
        for d in range(1, nz):
            relay(a, d)
    for d in range(1, nx):
        arrived(xin.at[xsrc(d), c], *s1[d], xpeer(d))
        send(xin.at[xsrc(d), c], xin.at[xsrc(d), c], *s2[d], cpeer)
    for d in range(nx):
        arrived(xin.at[xsrc(d), 1 - c], *s2[d], cpeer)
    for d in range(nz):
        complete(0, d)

    kdim = gs.shape[0]
    pre = jnp.dot(
        xin[...].reshape(seq, D), gsb[...].reshape(nz * ny * kdim, 2 * C), preferred_element_type=F32
    )
    branch_gate = jax.nn.gelu(pre[:, :C])
    branch_signal = jax.nn.gelu(pre[:, C:])
    total = jnp.sum(branch_signal, axis=1, keepdims=True)
    square = jnp.sum(branch_signal * branch_signal, axis=1, keepdims=True)
    lane = lax.broadcasted_iota(jnp.int32, (seq, LANES), 1)
    stat[0] = jnp.where(lane == 0, total, square).T[:8]
    sc = tsem()
    send(stat.at[0], stat.at[1], *sc, cpeer)
    arrived(stat.at[1], *sc, cpeer)
    stat[2] = stat[0] + stat[1]
    sx = [tsem() for _ in range(nx)]
    for d in range(1, nx):
        send(stat.at[2], stat.at[2 + d], *sx[d], xpeer(d))
    for d in range(1, nx):
        arrived(stat.at[2 + d], *sx[d], xpeer(d))
    summed = stat[2]
    for d in range(1, nx):
        summed = summed + stat[2 + d]
    back = summed.T
    row_mean = back[:, 0:1] / MIX_WIDTH
    spread = back[:, 1:2] / MIX_WIDTH - row_mean * row_mean
    spatial_input = (
        (branch_signal - row_mean) * lax.rsqrt(spread + EPSILON) * sgain[...].astype(F32)
    ).astype(BF16)
    rows_i = lax.broadcasted_iota(jnp.int32, (BLOCK, BLOCK), 0) // SEGMENT
    cols_i = lax.broadcasted_iota(jnp.int32, (BLOCK, BLOCK), 1) // SEGMENT
    own = spatial[t * C // HEAD_SIZE]
    own = jnp.where(cols_i <= rows_i, own, jnp.zeros_like(own))
    for d in range(nz):
        complete(1, d)
    per = BLOCK // R if R < BLOCK else 1
    gated = jnp.concatenate(
        [
            branch_gate[b * BLOCK:(b + 1) * BLOCK]
            * jnp.dot(own, spatial_input[b * BLOCK:(b + 1) * BLOCK], preferred_element_type=F32)
            for b in range(seq // BLOCK)
        ],
        axis=0,
    ).astype(BF16)
    for k in range(nz * ny):
        part = jnp.dot(gated, mob[k // ny, k % ny], preferred_element_type=F32).astype(BF16)
        for b in range(nx * 2):
            pm[b % 2, b // 2, :, k * cw:(k + 1) * cw] = part[b * R:(b + 1) * R]
    sc = tsem()
    send(pm.at[1 - c], prc, *sc, cpeer)
    arrived(prc, *sc, cpeer)
    for b in range(nx):
        abm[b] = (pm[c, b].astype(F32) + prc[b].astype(F32)).astype(BF16)
    sx = [tsem() for _ in range(nx)]
    for d in range(1, nx):
        send(abm.at[lax.rem(x + d, nx)], pxr.at[d - 1], *sx[d], xpeer(d))
    relay(2, 1)
    for d in range(1, nx):
        arrived(pxr.at[d - 1], *sx[d], xpeer(d))
    mix_out = pm[c, x].astype(F32) + prc[x].astype(F32)
    for d in range(1, nx):
        mix_out = mix_out + pxr[d - 1].astype(F32)
    mid[...] = (
        normalize(RESIDUAL_SCALE * tok[...].astype(F32) + mix_out) * mgain[...].astype(F32)
    ).astype(BF16)
    hin[q, x, c] = normalize(mid[...].astype(F32)).astype(BF16)

    sp = tsem()
    send(hin.at[q, x, c], hin.at[q, x, c], *sp, ppeer)
    sx = [[tsem() for _ in range(nx)] for _ in range(2)]
    sy = [[tsem() for _ in range(nx)] for _ in range(2)]
    for d in range(1, nx):
        send(hin.at[q, x, c], hin.at[q, x, c], *sx[0][d], xpeer(d))
    send(hin.at[q, x, c], hin.at[q, x, c], *sy[0][0], cpeer)
    issue(3)
    for d in range(2, nz):
        relay(2, d)
    arrived(hin.at[1 - q, x, c], *sp, ppeer)
    for d in range(1, nx):
        send(hin.at[1 - q, x, c], hin.at[1 - q, x, c], *sx[1][d], xpeer(d))
    send(hin.at[1 - q, x, c], hin.at[1 - q, x, c], *sy[1][0], cpeer)
    for k, s in enumerate((q, 1 - q)):
        for d in range(1, nx):
            arrived(hin.at[s, xsrc(d), c], *sx[k][d], xpeer(d))
            send(hin.at[s, xsrc(d), c], hin.at[s, xsrc(d), c], *sy[k][d], cpeer)
    for k, s in enumerate((q, 1 - q)):
        for d in range(nx):
            arrived(hin.at[s, xsrc(d), 1 - c], *sy[k][d], cpeer)
    for d in range(nz):
        complete(2, d)

    for s in range(2):

        def column(j, carry):
            at = pl.multiple_of(j * LANES, LANES)
            at_v = pl.multiple_of(W + j * LANES, LANES)
            lhs = hin[s].reshape(seq, D)
            wg = gvb[:, :, :, pl.ds(at, LANES)].reshape(D, LANES)
            wv = gvb[:, :, :, pl.ds(at_v, LANES)].reshape(D, LANES)
            both = jnp.dot(lhs, jnp.concatenate([wg, wv], axis=1), preferred_element_type=F32)
            gate = both[:, :LANES]
            value = both[:, LANES:]
            tap = taps[:, pl.ds(at, LANES)].astype(F32)
            row = lax.broadcasted_iota(jnp.int32, gate.shape, 0)
            one = jnp.where(row >= 1, pltpu.roll(gate, 1, 0), 0.0)
            two = jnp.where(row >= 2, pltpu.roll(gate, 2, 0), 0.0)
            conv = tap[0:1] * two + tap[1:2] * one + tap[2:3] * gate
            hid[s, :, pl.ds(at, LANES)] = (jax.nn.silu(conv) * value).astype(BF16)
            return carry

        lax.fori_loop(0, W // LANES, column, 0)

    sc = [tsem() for _ in range(nz)]
    sx = [[tsem() for _ in range(nx)] for _ in range(nz)]
    sz = [tsem() for _ in range(nz)]

    def down(i):
        g = zsrc(i)
        for s in range(2):
            for yy in range(ny):
                part = jnp.dot(hid[s], dnb[g, yy], preferred_element_type=F32).astype(BF16)
                for b in range(nx * 2):
                    pb[b % 2, g, b // 2, s, :, yy * cw:(yy + 1) * cw] = part[b * R:(b + 1) * R]
        send(pb.at[1 - c, g], rb.at[i], *sc[i], cpeer)

    def over_x(i):
        g = zsrc(i)
        arrived(rb.at[i], *sc[i], cpeer)
        for b in range(nx):
            for s in range(2):
                ab[i, b, s] = (pb[c, g, b, s].astype(F32) + rb[i, b, s].astype(F32)).astype(BF16)
        for d in range(1, nx):
            send(ab.at[i, lax.rem(x + d, nx)], xr.at[i, d - 1], *sx[i][d], xpeer(d))

    def over_z(i):
        g = zsrc(i)
        for d in range(1, nx):
            arrived(xr.at[i, d - 1], *sx[i][d], xpeer(d))
        for s in range(2):
            acc = ab[i, x, s].astype(F32)
            for d in range(1, nx):
                acc = acc + xr[i, d - 1, s].astype(F32)
            zb[g, s] = acc.astype(BF16)

    for d in range(1, nz):
        relay(3, d)
    for i in range(nz):
        complete(3, i)
        down(i)
        if i >= 1:
            over_x(i - 1)
        if i >= 2:
            over_z(i - 2)
    over_x(nz - 1)
    over_z(nz - 2)
    over_z(nz - 1)
    for g in range(nz):
        send(zb.at[g, 1 - q], zr.at[g], *sz[g], ppeer)
    for g in range(nz):
        arrived(zr.at[g], *sz[g], ppeer)
    ffn_out = jnp.concatenate(
        [zb[g, q].astype(F32) + zr[g].astype(F32) for g in range(nz)], axis=1
    )
    out[...] = (
        normalize(RESIDUAL_SCALE * mid[...].astype(F32) + ffn_out) * ogain[...].astype(F32)
    ).astype(BF16)
    for copy in pending:
        copy.wait_send()


def shards(nf, nt, ny, tokens, gate_proj, signal_proj, spatial, signal_gain, mixer_out, mixer_gain, ffn_gate, ffn_value, conv_taps, ffn_down, output_gain):
    nz = nf // ny
    nx = nt // 2
    R, D = tokens.shape
    C = gate_proj.shape[1]
    H = ffn_gate.shape[1]
    W = -(-H // (2 * LANES)) * LANES
    cw = mixer_out.shape[1]
    seq = nx * 2 * R
    q = (lax.axis_index("fs") // ny) % 2

    gs = jnp.concatenate([gate_proj, signal_proj], axis=1)
    gv = jnp.stack(
        [
            jnp.concatenate([ffn_gate[:, :W], ffn_value[:, :W]], axis=1),
            jnp.concatenate([ffn_gate[:, H - W:], ffn_value[:, H - W:]], axis=1),
        ]
    )
    fresh = (jnp.arange(W) >= 2 * W - H)[:, None]
    low = ffn_down[H - W:]
    dn = jnp.stack([ffn_down[:W], jnp.where(fresh, low, jnp.zeros_like(low))])
    taps = lax.dynamic_slice_in_dim(conv_taps, q * (H - W), W, 1)
    gw = ny * cw
    vm = functools.partial(pltpu.VMEM)
    dma = pltpu.SemaphoreType.DMA
    n_t = 2 * nx + 1 + nx + 1 + nx + 1 + 4 * nx + nz * (2 + nx)
    scratch = [
        vm((nz, ny) + gs.shape, BF16),
        vm((nz, ny) + mixer_out.shape, BF16),
        vm((nz, ny) + gv.shape[1:], BF16),
        vm((nz, ny) + dn.shape[1:], BF16),
        vm((nx, 2, R, D), BF16),
        vm((2 + nx, 8, seq), F32),
        vm((2, nx, R, D), BF16),
        vm((nx, R, D), BF16),
        vm((nx, R, D), BF16),
        vm((nx - 1, R, D), BF16),
        vm((R, D), BF16),
        vm((2, nx, 2, R, D), BF16),
        vm((2, seq, W), BF16),
        vm((2, nz, nx, 2, R, gw), BF16),
        vm((nz, nx, 2, R, gw), BF16),
        vm((nz, nx, 2, R, gw), BF16),
        vm((nz, nx - 1, 2, R, gw), BF16),
        vm((nz, 2, R, gw), BF16),
        vm((nz, R, gw), BF16),
        dma((4,)),
        dma((4, nz)),
        dma((4, nz)),
        dma((4, nz, ny)),
        dma((4, nz, ny)),
        dma((n_t,)),
        dma((n_t,)),
    ]
    return pl.pallas_call(
        functools.partial(kernel, nz, ny, nx),
        out_shape=jax.ShapeDtypeStruct((R, D), BF16),
        in_specs=[pl.BlockSpec(memory_space=pltpu.VMEM)] * 10,
        out_specs=pl.BlockSpec(memory_space=pltpu.VMEM),
        scratch_shapes=scratch,
        compiler_params=pltpu.CompilerParams(
            collective_id=0, has_side_effects=True, vmem_limit_bytes=67043328
        ),
    )(
        tokens, gs, mixer_out, gv, dn, spatial, signal_gain[None], mixer_gain[None], taps, output_gain[None]
    )


def solution(mesh):
    nf, nt = mesh.shape["fs"], mesh.shape["tp"]
    ny = 2 ** (int(math.log2(nf // 2)) // 2)
    in_specs = (
        P(("fs", "tp"), None),
        P("fs", "tp"),
        P("fs", "tp"),
        P(),
        P("tp"),
        P("tp", "fs"),
        P(),
        P("fs", "tp"),
        P("fs", "tp"),
        P(None, "tp"),
        P("tp", "fs"),
        P(),
    )
    return jax.shard_map(
        functools.partial(shards, nf, nt, ny),
        mesh=mesh,
        in_specs=in_specs,
        out_specs=P(("fs", "tp"), None),
        check_vma=False,
    )
```

```python
import functools
import math

import jax
import jax.numpy as jnp
from jax import lax
from jax.experimental import pallas as pl
from jax.experimental.pallas import tpu as pltpu
from jax.sharding import PartitionSpec as P

MIX_WIDTH = 512
HEAD_SIZE = 128
BLOCK = 128
SEGMENT = 64
LANES = 128
GV_PIECES = 4
DN_PIECES = 2
EPSILON = 1e-05
RESIDUAL_SCALE = math.sqrt(2.0)
MESH = pl.DeviceIdType.MESH
F32 = jnp.float32
BF16 = jnp.bfloat16


def normalize(values):
    row_mean = jnp.mean(values, axis=-1, keepdims=True)
    centred = values - row_mean
    spread = jnp.mean(centred * centred, axis=-1, keepdims=True)
    return centred * lax.rsqrt(spread + EPSILON)


def kernel(
    nz, ny, nx,
    tok, gs, mo, gv, dn, spatial, sgain, mgain, taps, ogain,
    out,
    gsb, mob, gvb, dnb, xin, stat, pm, prc, abm, pxr, mid, hin, hid, pb, rb, ab, xr, zb, zr,
    loc_sem, zs, zrs, ys, yrs, ts, trs,
):
    R, D = tok.shape
    C = mo.shape[0]
    cw = mo.shape[1]
    W = dn.shape[1]
    f = lax.axis_index("fs")
    t = lax.axis_index("tp")
    z, y = f // ny, f % ny
    x, c = t // 2, t % 2
    q = z % 2
    seq = nx * 2 * R

    def zpeer(d):
        return (lax.rem(z + d, nz) * ny + y, t)

    def ypeer(d):
        return (z * ny + lax.rem(y + d, ny), t)

    def xpeer(d):
        return (f, lax.rem(x + d, nx) * 2 + c)

    cpeer = (f, x * 2 + 1 - c)
    ppeer = ((z + 1 - 2 * q) * ny + y, t)

    def zsrc(d):
        return lax.rem(z + nz - d, nz)

    def ysrc(d):
        return lax.rem(y + ny - d, ny)

    def xsrc(d):
        return lax.rem(x + nx - d, nx)

    pending = []

    def send(src, dst, ssem, rsem, to):
        copy = pltpu.make_async_remote_copy(
            src_ref=src, dst_ref=dst, send_sem=ssem, recv_sem=rsem, device_id=to, device_id_type=MESH
        )
        copy.start()
        pending.append(copy)

    def arrived(dst, ssem, rsem, to):
        pltpu.make_async_remote_copy(
            src_ref=dst, dst_ref=dst, send_sem=ssem, recv_sem=rsem, device_id=to, device_id_type=MESH
        ).wait_recv()

    barrier = pltpu.get_barrier_semaphore()
    peers = [zpeer(d) for d in range(1, nz)] + [ypeer(d) for d in range(1, ny)]
    peers += [xpeer(d) for d in range(1, nx)] + [cpeer]
    for p in peers:
        pl.semaphore_signal(barrier, inc=1, device_id=p, device_id_type=MESH)
    pl.semaphore_wait(barrier, len(peers))

    gv_rows = gv.shape[1] // GV_PIECES
    dn_rows = W // DN_PIECES
    DN = 2 + GV_PIECES
    EARLY = DN - 2

    def slot(a, zz, yy):
        if a == 0:
            return gsb.at[zz, yy]
        if a == 1:
            return mob.at[zz, yy]
        if a < DN:
            return gvb.at[zz, yy, pl.ds((a - 2) * gv_rows, gv_rows)]
        return dnb.at[zz, yy, pl.ds((a - DN) * dn_rows, dn_rows)]

    def local(a, zz):
        if a == 0:
            return gs
        if a == 1:
            return mo
        if a < DN:
            return gv.at[zz % 2, pl.ds((a - 2) * gv_rows, gv_rows)]
        return dn.at[zz % 2, pl.ds((a - DN) * dn_rows, dn_rows)]

    def issue(a):
        own = pltpu.make_async_copy(local(a, z), slot(a, z, y), loc_sem.at[a])
        own.start()
        for d in range(1, nz):
            to = zpeer(d)
            send(local(a, lax.rem(z + d, nz)), slot(a, z, y), zs.at[a, d], zrs.at[a, d], to)
        for e in range(1, ny):
            send(local(a, z), slot(a, z, y), ys.at[a, 0, e], yrs.at[a, 0, e], ypeer(e))
        own.wait()

    def relay(a):
        for d in range(1, nz):
            zz = zsrc(d)
            arrived(slot(a, zz, y), zs.at[a, d], zrs.at[a, d], zpeer(d))
            for e in range(1, ny):
                send(slot(a, zz, y), slot(a, zz, y), ys.at[a, d, e], yrs.at[a, d, e], ypeer(e))

    def complete(a, d):
        zz = zsrc(d)
        for e in range(1, ny):
            yy = ysrc(e)
            arrived(slot(a, zz, yy), ys.at[a, d, e], yrs.at[a, d, e], ypeer(e))

    scope = jax.named_scope

    tslot = [0]

    def tsem():
        k = tslot[0]
        tslot[0] += 1
        return ts.at[k], trs.at[k]

    issue(0)
    issue(1)

    xin[x, c] = normalize(tok[...].astype(F32)).astype(BF16)
    s1 = [tsem() for _ in range(nx)]
    s2 = [tsem() for _ in range(nx)]
    for d in range(1, nx):
        send(xin.at[x, c], xin.at[x, c], *s1[d], xpeer(d))
    send(xin.at[x, c], xin.at[x, c], *s2[0], cpeer)
    with scope("relay_mix"):
        relay(0)
        relay(1)
    for a in range(2, EARLY):
        issue(a)
    for d in range(1, nx):
        arrived(xin.at[xsrc(d), c], *s1[d], xpeer(d))
        send(xin.at[xsrc(d), c], xin.at[xsrc(d), c], *s2[d], cpeer)
    for d in range(nx):
        arrived(xin.at[xsrc(d), 1 - c], *s2[d], cpeer)
    with scope("complete_gs"):
        for d in range(nz):
            complete(0, d)

    kdim = gs.shape[0]
    pre = jnp.dot(
        xin[...].reshape(seq, D), gsb[...].reshape(nz * ny * kdim, 2 * C), preferred_element_type=F32
    )
    branch_gate = jax.nn.gelu(pre[:, :C])
    branch_signal = jax.nn.gelu(pre[:, C:])
    total = jnp.sum(branch_signal, axis=1, keepdims=True)
    square = jnp.sum(branch_signal * branch_signal, axis=1, keepdims=True)
    lane = lax.broadcasted_iota(jnp.int32, (seq, LANES), 1)
    stat[0] = jnp.where(lane == 0, total, square).T[:8]
    sc = tsem()
    send(stat.at[0], stat.at[1], *sc, cpeer)
    arrived(stat.at[1], *sc, cpeer)
    stat[2] = stat[0] + stat[1]
    sx = [tsem() for _ in range(nx)]
    for d in range(1, nx):
        send(stat.at[2], stat.at[2 + d], *sx[d], xpeer(d))
    for d in range(1, nx):
        arrived(stat.at[2 + d], *sx[d], xpeer(d))
    summed = stat[2]
    for d in range(1, nx):
        summed = summed + stat[2 + d]
    back = summed.T
    row_mean = back[:, 0:1] / MIX_WIDTH
    spread = back[:, 1:2] / MIX_WIDTH - row_mean * row_mean
    spatial_input = (
        (branch_signal - row_mean) * lax.rsqrt(spread + EPSILON) * sgain[...].astype(F32)
    ).astype(BF16)
    rows_i = lax.broadcasted_iota(jnp.int32, (BLOCK, BLOCK), 0) // SEGMENT
    cols_i = lax.broadcasted_iota(jnp.int32, (BLOCK, BLOCK), 1) // SEGMENT
    own = spatial[t * C // HEAD_SIZE]
    own = jnp.where(cols_i <= rows_i, own, jnp.zeros_like(own))
    with scope("complete_mo"):
        for d in range(nz):
            complete(1, d)
    gated = jnp.concatenate(
        [
            branch_gate[b * BLOCK:(b + 1) * BLOCK]
            * jnp.dot(own, spatial_input[b * BLOCK:(b + 1) * BLOCK], preferred_element_type=F32)
            for b in range(seq // BLOCK)
        ],
        axis=0,
    ).astype(BF16)
    for k in range(nz * ny):
        part = jnp.dot(gated, mob[k // ny, k % ny], preferred_element_type=F32).astype(BF16)
        for b in range(nx * 2):
            pm[b % 2, b // 2, :, k * cw:(k + 1) * cw] = part[b * R:(b + 1) * R]
    sc = tsem()
    send(pm.at[1 - c], prc, *sc, cpeer)
    arrived(prc, *sc, cpeer)
    for b in range(nx):
        abm[b] = (pm[c, b].astype(F32) + prc[b].astype(F32)).astype(BF16)
    sx = [tsem() for _ in range(nx)]
    for d in range(1, nx):
        send(abm.at[lax.rem(x + d, nx)], pxr.at[d - 1], *sx[d], xpeer(d))
    with scope("mix_x"):
        for d in range(1, nx):
            arrived(pxr.at[d - 1], *sx[d], xpeer(d))
    mix_out = pm[c, x].astype(F32) + prc[x].astype(F32)
    for d in range(1, nx):
        mix_out = mix_out + pxr[d - 1].astype(F32)
    mid[...] = (
        normalize(RESIDUAL_SCALE * tok[...].astype(F32) + mix_out) * mgain[...].astype(F32)
    ).astype(BF16)
    hin[q, x, c] = normalize(mid[...].astype(F32)).astype(BF16)

    sp = tsem()
    send(hin.at[q, x, c], hin.at[q, x, c], *sp, ppeer)
    sx = [[tsem() for _ in range(nx)] for _ in range(2)]
    sy = [[tsem() for _ in range(nx)] for _ in range(2)]
    for d in range(1, nx):
        send(hin.at[q, x, c], hin.at[q, x, c], *sx[0][d], xpeer(d))
    send(hin.at[q, x, c], hin.at[q, x, c], *sy[0][0], cpeer)
    for a in range(EARLY, DN + DN_PIECES):
        issue(a)
    for a in range(2, DN - 1):
        with scope(f"relay_gv{a - 2}"):
            relay(a)
    with scope("relay_gv3"):
        relay(DN - 1)
    with scope("pair_rows"):
        arrived(hin.at[1 - q, x, c], *sp, ppeer)
    for d in range(1, nx):
        send(hin.at[1 - q, x, c], hin.at[1 - q, x, c], *sx[1][d], xpeer(d))
    send(hin.at[1 - q, x, c], hin.at[1 - q, x, c], *sy[1][0], cpeer)
    with scope("rows_x"):
        for k, s in enumerate((q, 1 - q)):
            for d in range(1, nx):
                arrived(hin.at[s, xsrc(d), c], *sx[k][d], xpeer(d))
                send(hin.at[s, xsrc(d), c], hin.at[s, xsrc(d), c], *sy[k][d], cpeer)
    with scope("rows_core"):
        for k, s in enumerate((q, 1 - q)):
            for d in range(nx):
                arrived(hin.at[s, xsrc(d), 1 - c], *sy[k][d], cpeer)
    with scope("relay_dn0"):
        relay(DN)
    with scope("complete_gv"):
        for a in range(2, DN):
            for d in range(nz):
                complete(a, d)

    for s in range(2):

        def column(j, carry):
            at = pl.multiple_of(j * LANES, LANES)
            at_v = pl.multiple_of(W + j * LANES, LANES)
            lhs = hin[s].reshape(seq, D)
            wg = gvb[:, :, :, pl.ds(at, LANES)].reshape(D, LANES)
            wv = gvb[:, :, :, pl.ds(at_v, LANES)].reshape(D, LANES)
            both = jnp.dot(lhs, jnp.concatenate([wg, wv], axis=1), preferred_element_type=F32)
            gate = both[:, :LANES]
            value = both[:, LANES:]
            tap = taps[q, :, pl.ds(at, LANES)].astype(F32)
            row = lax.broadcasted_iota(jnp.int32, gate.shape, 0)
            one = jnp.where(row >= 1, pltpu.roll(gate, 1, 0), 0.0)
            two = jnp.where(row >= 2, pltpu.roll(gate, 2, 0), 0.0)
            conv = tap[0:1] * two + tap[1:2] * one + tap[2:3] * gate
            hid[s, :, pl.ds(at, LANES)] = (jax.nn.silu(conv) * value).astype(BF16)
            return carry

        with scope("gate_value"):
            lax.fori_loop(0, W // LANES, column, 0)
        if s == 0:
            with scope("relay_dn1"):
                for a in range(DN + 1, DN + DN_PIECES):
                    relay(a)

    sc = [[tsem() for _ in range(2)] for _ in range(nz)]
    sx = [[[tsem() for _ in range(nx)] for _ in range(2)] for _ in range(nz)]
    zbase = tslot[0]
    tslot[0] += nz
    turns = (1 - q, q)

    def down(i):
        g = zsrc(i)
        for k, s in enumerate(turns):
            for yy in range(ny):
                part = jnp.dot(hid[s], dnb[g, yy], preferred_element_type=F32).astype(BF16)
                for b in range(nx * 2):
                    pb[b % 2, g, s, b // 2, :, yy * cw:(yy + 1) * cw] = part[b * R:(b + 1) * R]
            send(pb.at[1 - c, g, s], rb.at[i, s], *sc[i][k], cpeer)

    def over_x(i):
        g = zsrc(i)
        for k, s in enumerate(turns):
            arrived(rb.at[i, s], *sc[i][k], cpeer)
            for b in range(nx):
                ab[i, s, b] = (pb[c, g, s, b].astype(F32) + rb[i, s, b].astype(F32)).astype(BF16)
            for d in range(1, nx):
                send(ab.at[i, s, lax.rem(x + d, nx)], xr.at[i, d - 1, s], *sx[i][k][d], xpeer(d))

    def over_z(i):
        g = zsrc(i)
        for k, s in enumerate(turns):
            for d in range(1, nx):
                arrived(xr.at[i, d - 1, s], *sx[i][k][d], xpeer(d))
            acc = ab[i, s, x].astype(F32)
            for d in range(1, nx):
                acc = acc + xr[i, d - 1, s].astype(F32)
            zb[g, s] = acc.astype(BF16)
            if k == 0:
                send(zb.at[g, s], zr.at[g], ts.at[zbase + g], trs.at[zbase + g], ppeer)

    for i in range(nz):
        with scope(f"complete_dn{i}"):
            for a in range(DN, DN + DN_PIECES):
                complete(a, i)
        with scope(f"down{i}"):
            down(i)
        if i >= 1:
            over_x(i - 1)
        if i >= 2:
            over_z(i - 2)
    with scope("tail_x"):
        over_x(nz - 1)
        over_z(nz - 2)
        over_z(nz - 1)
    with scope("tail_z"):
        for g in range(nz):
            arrived(zr.at[g], ts.at[zbase + g], trs.at[zbase + g], ppeer)
    ffn_out = jnp.concatenate(
        [zb[g, q].astype(F32) + zr[g].astype(F32) for g in range(nz)], axis=1
    )
    out[...] = (
        normalize(RESIDUAL_SCALE * mid[...].astype(F32) + ffn_out) * ogain[...].astype(F32)
    ).astype(BF16)
    for copy in pending:
        copy.wait_send()


def shards(nf, nt, ny, tokens, gate_proj, signal_proj, spatial, signal_gain, mixer_out, mixer_gain, ffn_gate, ffn_value, conv_taps, ffn_down, output_gain):
    nz = nf // ny
    nx = nt // 2
    R, D = tokens.shape
    C = gate_proj.shape[1]
    H = ffn_gate.shape[1]
    W = -(-H // (2 * LANES)) * LANES
    cw = mixer_out.shape[1]
    seq = nx * 2 * R

    gs = jnp.concatenate([gate_proj, signal_proj], axis=1)
    gv = jnp.stack(
        [
            jnp.concatenate([ffn_gate[:, :W], ffn_value[:, :W]], axis=1),
            jnp.concatenate([ffn_gate[:, H - W:], ffn_value[:, H - W:]], axis=1),
        ]
    )
    fresh = (jnp.arange(W) >= 2 * W - H)[:, None]
    low = ffn_down[H - W:]
    dn = jnp.stack([ffn_down[:W], jnp.where(fresh, low, jnp.zeros_like(low))])
    taps = jnp.stack([conv_taps[:, :W], conv_taps[:, H - W:]])
    gw = ny * cw
    vm = pltpu.VMEM
    n_w = 2 + GV_PIECES + DN_PIECES
    dma = pltpu.SemaphoreType.DMA
    n_t = 2 * nx + 1 + nx + 1 + nx + 1 + 4 * nx + nz * (3 + 2 * nx)
    scratch = [
        vm((nz, ny) + gs.shape, BF16),
        vm((nz, ny) + mixer_out.shape, BF16),
        vm((nz, ny) + gv.shape[1:], BF16),
        vm((nz, ny) + dn.shape[1:], BF16),
        vm((nx, 2, R, D), BF16),
        vm((2 + nx, 8, seq), F32),
        vm((2, nx, R, D), BF16),
        vm((nx, R, D), BF16),
        vm((nx, R, D), BF16),
        vm((nx - 1, R, D), BF16),
        vm((R, D), BF16),
        vm((2, nx, 2, R, D), BF16),
        vm((2, seq, W), BF16),
        vm((2, nz, 2, nx, R, gw), BF16),
        vm((nz, 2, nx, R, gw), BF16),
        vm((nz, 2, nx, R, gw), BF16),
        vm((nz, nx - 1, 2, R, gw), BF16),
        vm((nz, 2, R, gw), BF16),
        vm((nz, R, gw), BF16),
        dma((n_w,)),
        dma((n_w, nz)),
        dma((n_w, nz)),
        dma((n_w, nz, ny)),
        dma((n_w, nz, ny)),
        dma((n_t,)),
        dma((n_t,)),
    ]
    return pl.pallas_call(
        functools.partial(kernel, nz, ny, nx),
        out_shape=jax.ShapeDtypeStruct((R, D), BF16),
        in_specs=[pl.BlockSpec(memory_space=pltpu.VMEM)] * 10,
        out_specs=pl.BlockSpec(memory_space=pltpu.VMEM),
        scratch_shapes=scratch,
        compiler_params=pltpu.CompilerParams(
            collective_id=0, has_side_effects=True, vmem_limit_bytes=67043328
        ),
    )(
        tokens, gs, mixer_out, gv, dn, spatial, signal_gain[None], mixer_gain[None], taps, output_gain[None]
    )


def solution(mesh):
    nf, nt = mesh.shape["fs"], mesh.shape["tp"]
    ny = 2 ** (int(math.log2(nf // 2)) // 2)
    in_specs = (
        P(("fs", "tp"), None),
        P("fs", "tp"),
        P("fs", "tp"),
        P(),
        P("tp"),
        P("tp", "fs"),
        P(),
        P("fs", "tp"),
        P("fs", "tp"),
        P(None, "tp"),
        P("tp", "fs"),
        P(),
    )
    return jax.shard_map(
        functools.partial(shards, nf, nt, ny),
        mesh=mesh,
        in_specs=in_specs,
        out_specs=P(("fs", "tp"), None),
        check_vma=False,
    )
```
